32 devices in a mesh: sp: 8 (over z, y), tp: 4 (over x, core).
Axes of the slice: x: 2, y: 2, z: 4, core: 2. Of those that a mesh axis runs over, the one named last changes fastest.
Arguments:
- grouped_head_inputs: bfloat16 [8192, 2, 1024], P('sp', None, 'tp'), may hold values from -6 to 6
- head_gate_inputs: bfloat16 [8192, 2, 1024], P('sp', None, 'tp'), may hold values from -6 to 6
- unsmoothed_step: float32 [8192, 2, 16], P('sp', None, 'tp'), may hold values from -3.8 to 3.8
- head_decay_rate: float32 [2, 16], P(None, 'tp'), may hold values from 1.2207031e-05 to 0.04761905
- extra_log_decay: float32 [8192, 2, 16], P('sp', None, 'tp'), may hold values from -1.4 to 0
- first_group_keys: bfloat16 [8192, 128], P('sp'), may hold values from -6 to 6
- first_group_queries: bfloat16 [8192, 128], P('sp'), may hold values from -6 to 6
- second_group_keys: bfloat16 [8192, 64], P('sp'), may hold values from -6 to 6
- second_group_queries: bfloat16 [8192, 64], P('sp'), may hold values from -6 to 6
- head_input_filter: float32 [4, 2, 1024], P(None, None, 'tp'), may hold values from -3 to 3
- first_group_filter: float32 [4, 2, 128], replicated, may hold values from -3 to 3
- second_group_filter: float32 [4, 2, 64], replicated, may hold values from -3 to 3
- head_norm_gain: float32 [2, 1024], P(None, 'tp'), may hold values from 0.1 to 1.9
- output_weight: bfloat16 [2, 1024, 2048], P(None, None, 'tp'), may hold values from -0.125 to 0.125
- residual: bfloat16 [8192, 2048], P('sp', 'tp'), may hold values from -37 to 37
- channel_norm_gain: float32 [2048], replicated, may hold values from 0.1 to 1.9
- channel_gate_weight: bfloat16 [2048, 5120], P('sp', 'tp'), may hold values from -0.125 to 0.125
- channel_up_weight: bfloat16 [2048, 5120], P('sp', 'tp'), may hold values from -0.125 to 0.125
- channel_down_weight: bfloat16 [2048, 5120], P('sp', 'tp'), may hold values from -0.078125 to 0.078125
Outputs:
- layer_output: bfloat16 [8192, 2048], P('sp', 'tp')
The draws below stay inside these ranges and needn't reach their ends.
All inputs are finite; a program needn't handle non-finite values.
Results may differ from the reference program's by a relative error of at most 0.007.
Values may be sent and summed in bfloat16 or wider, within the bound.
A program may use at most 128 MiB of HBM per device.

```python
import math
import jax
import jax.numpy as jnp
from jax import lax

D = 2048
GROUP_HEADS = 16
HEAD = 64
STATE_ONE = 128
STATE_TWO = 64
FF = 5120
CONV = 4
BLOCK = 128
TOKENS = 8192
CHANNELS = 1024
N_TP = 4


def draw_unsmoothed_step(key, part):
    noise_key = jax.random.fold_in(key, 11)
    block_key = jax.random.fold_in(key, 12)
    block_total = TOKENS // BLOCK
    offsets = jax.random.uniform(block_key, (block_total, 1, 1, 1), jnp.float32, -1.0, 1.0)
    noise = 0.7 * jax.random.truncated_normal(noise_key, -4.0, 4.0, (block_total, BLOCK, 2, GROUP_HEADS), jnp.float32)
    return (noise + offsets).reshape(TOKENS, 2, GROUP_HEADS)


def draw_head_decay_rate(key, part):
    choose_key = jax.random.fold_in(key, 21)
    fast_key = jax.random.fold_in(key, 22)
    slow_key = jax.random.fold_in(key, 23)
    share = 0.5
    quick = jax.random.uniform(choose_key, (2, GROUP_HEADS), jnp.float32) < share
    fast = jnp.exp(jax.random.uniform(fast_key, (2, GROUP_HEADS), jnp.float32, math.log(1.0 / 70.0), math.log(1.0 / 21.0)))
    slow = jnp.exp(jax.random.uniform(slow_key, (2, GROUP_HEADS), jnp.float32, math.log(0.1), math.log(0.6))) / TOKENS
    return jnp.where(quick, fast, slow)


def draw_extra_log_decay(key, part):
    place_key = jax.random.fold_in(key, 31)
    loss_key = jax.random.fold_in(key, 32)
    places = jax.random.randint(place_key, (2, 2, GROUP_HEADS), 0, TOKENS)
    losses = jax.random.uniform(loss_key, (2, 2, GROUP_HEADS), jnp.float32, 0.2, 0.5)
    positions = jnp.arange(TOKENS, dtype=jnp.int32)[:, None, None, None]
    struck = positions == places[None]
    return jnp.sum(jnp.where(struck, jnp.log(1.0 - losses)[None], 0.0), axis=1)


def draw_residual(key, part):
    row_key = jax.random.fold_in(key, 41)
    column_key = jax.random.fold_in(key, 42)
    noise_key = jax.random.fold_in(key, 43)
    row_scale = jnp.exp(jax.random.uniform(row_key, (TOKENS, 1), jnp.float32, math.log(0.3), math.log(3.0)))
    column_scale = jnp.exp(jax.random.uniform(column_key, (1, D), jnp.float32, math.log(0.3), math.log(3.0)))
    noise = jax.random.truncated_normal(noise_key, -4.0, 4.0, (TOKENS, D), jnp.float32)
    return (noise * row_scale * column_scale).astype(jnp.bfloat16)


def level_of(own_key, dims, cuts, least, high):
    def one(axis_at, parts):
        heights = jax.random.uniform(jax.random.fold_in(jax.random.fold_in(own_key, 6), axis_at), (parts,), jnp.float32, least / len(cuts), high / len(cuts))
        return jnp.repeat(jnp.exp(heights), dims[axis_at] // parts).reshape((-1,) + (1,) * (len(dims) - axis_at - 1))

    gain = one(*cuts[0])
    for cut in cuts[1:]:
        gain = gain * one(*cut)
    return gain


def normal_values(own_key, dims, width, bound, cuts=(), kind=jnp.bfloat16):
    level = level_of(own_key, dims, cuts, -0.22, 0.18) if cuts else 1.0
    entries = jax.random.normal(own_key, dims, jnp.float32) * width * level
    return jnp.minimum(jnp.maximum(entries, -bound), bound).astype(kind)


def setup_inputs(seed: int = 0) -> dict:
    key_list = jax.random.split(jax.random.key(seed), 20)
    grouped_head_inputs = normal_values(key_list[0], (TOKENS, 2, CHANNELS), 1.0, 6.0, ((0, 8), (2, 4)))
    head_gate_inputs = normal_values(key_list[1], (TOKENS, 2, CHANNELS), 1.0, 6.0, ((0, 8), (2, 4)))
    unsmoothed_step = draw_unsmoothed_step(jax.random.fold_in(key_list[19], 71), 0)
    head_decay_rate = draw_head_decay_rate(jax.random.fold_in(key_list[19], 71), 0)
    extra_log_decay = draw_extra_log_decay(jax.random.fold_in(key_list[19], 71), 0)
    first_group_keys = normal_values(key_list[5], (TOKENS, STATE_ONE), 1.0, 6.0, ((0, 8),))
    first_group_queries = normal_values(key_list[6], (TOKENS, STATE_ONE), 1.0, 6.0, ((0, 8),))
    second_group_keys = normal_values(key_list[7], (TOKENS, STATE_TWO), 1.0, 6.0, ((0, 8),))
    second_group_queries = normal_values(key_list[8], (TOKENS, STATE_TWO), 1.0, 6.0, ((0, 8),))
    head_input_filter = normal_values(key_list[9], (CONV, 2, CHANNELS), 0.5, 3.0, ((2, 4),), jnp.float32)
    first_group_filter = normal_values(key_list[10], (CONV, 2, STATE_ONE), 0.5, 3.0, (), jnp.float32)
    second_group_filter = normal_values(key_list[11], (CONV, 2, STATE_TWO), 0.5, 3.0, (), jnp.float32)
    head_norm_gain = jnp.clip(1.0 + 0.18 * jax.random.normal(key_list[12], (2, CHANNELS), jnp.float32), 0.1, 1.9)
    output_weight = normal_values(key_list[13], (2, CHANNELS, D), (2 * CHANNELS) ** -0.5, 0.125, ((2, 4),))
    residual = draw_residual(jax.random.fold_in(key_list[19], 71), 0)
    channel_norm_gain = jnp.clip(1.0 + 0.18 * jax.random.normal(key_list[15], (D,), jnp.float32), 0.1, 1.9)
    channel_gate_weight = normal_values(key_list[16], (D, FF), D ** -0.5, 0.125, ((0, 8), (1, 4)))
    channel_up_weight = normal_values(key_list[17], (D, FF), D ** -0.5, 0.125, ((0, 8), (1, 4)))
    channel_down_weight = normal_values(key_list[18], (D, FF), FF ** -0.5, 0.078125, ((0, 8), (1, 4)))
    return dict(grouped_head_inputs=grouped_head_inputs, head_gate_inputs=head_gate_inputs, unsmoothed_step=unsmoothed_step, head_decay_rate=head_decay_rate, extra_log_decay=extra_log_decay, first_group_keys=first_group_keys, first_group_queries=first_group_queries, second_group_keys=second_group_keys, second_group_queries=second_group_queries, head_input_filter=head_input_filter, first_group_filter=first_group_filter, second_group_filter=second_group_filter, head_norm_gain=head_norm_gain, output_weight=output_weight, residual=residual, channel_norm_gain=channel_norm_gain, channel_gate_weight=channel_gate_weight, channel_up_weight=channel_up_weight, channel_down_weight=channel_down_weight)


EPSILON = 1e-06
PRECISE = lax.Precision.HIGHEST

def causal_taps(values, taps):
    length = values.shape[0]
    zeros_rows = jnp.zeros((CONV - 1,) + values.shape[1:], jnp.float32)
    padded = jnp.concatenate([zeros_rows, values.astype(jnp.float32)], axis=0)
    running = jnp.zeros(values.shape, jnp.float32)
    for offset in range(CONV):
        running = running + taps[offset].astype(jnp.float32) * padded[offset:offset + length]
    return jax.nn.silu(running)

def block_pass(current, value_rows, log_rows, key_rows, query_rows):
    cumulative = jnp.cumsum(log_rows, axis=0)
    length = value_rows.shape[0]
    causal = jnp.arange(length)[:, None] >= jnp.arange(length)[None, :]
    scores = jnp.dot(query_rows, key_rows.T, precision=PRECISE)
    span_logs = jnp.where(causal[:, :, None], cumulative[:, None, :] - cumulative[None, :, :], -jnp.inf)
    weights = jnp.exp(span_logs) * scores[:, :, None]
    inside = jnp.einsum('lsh,shp->lhp', weights, value_rows, precision=PRECISE)
    carried = jnp.einsum('ls,hps->lhp', query_rows, current, precision=PRECISE) * jnp.exp(cumulative)[:, :, None]
    to_end = jnp.exp(cumulative[-1][None, :] - cumulative)
    update = jnp.einsum('lhp,ls->hps', value_rows * to_end[:, :, None], key_rows, precision=PRECISE)
    new_state = current * jnp.exp(cumulative[-1])[:, None, None] + update
    return (new_state, inside + carried)

def scan_group(value_rows, log_rows, key_rows, query_rows):
    length, head_count, head_width = value_rows.shape
    block_count = length // BLOCK
    initial = jnp.zeros((head_count, head_width, key_rows.shape[1]), jnp.float32)
    blocks = (value_rows.reshape(block_count, BLOCK, head_count, head_width), log_rows.reshape(block_count, BLOCK, head_count), key_rows.reshape(block_count, BLOCK, -1), query_rows.reshape(block_count, BLOCK, -1))

    def advance(current, pieces):
        return block_pass(current, pieces[0], pieces[1], pieces[2], pieces[3])
    final_state, outputs = lax.scan(advance, initial, blocks)
    return outputs.reshape(length, head_count, head_width)

def reference(grouped_head_inputs, head_gate_inputs, unsmoothed_step, head_decay_rate, extra_log_decay, first_group_keys, first_group_queries, second_group_keys, second_group_queries, head_input_filter, first_group_filter, second_group_filter, head_norm_gain, output_weight, residual, channel_norm_gain, channel_gate_weight, channel_up_weight, channel_down_weight):
    length = grouped_head_inputs.shape[0]
    conv_heads = causal_taps(grouped_head_inputs, head_input_filter)
    keys_one = causal_taps(first_group_keys, first_group_filter[:, 0])
    queries_one = causal_taps(first_group_queries, first_group_filter[:, 1])
    keys_two = causal_taps(second_group_keys, second_group_filter[:, 0])
    queries_two = causal_taps(second_group_queries, second_group_filter[:, 1])
    head_step_size = jax.nn.softplus(unsmoothed_step.astype(jnp.float32))
    decay_logarithm = extra_log_decay.astype(jnp.float32) - head_step_size * head_decay_rate.astype(jnp.float32)[None]
    values = conv_heads.reshape(length, 2, GROUP_HEADS, HEAD) * head_step_size[:, :, :, None]
    first = scan_group(values[:, 0], decay_logarithm[:, 0], keys_one, queries_one)
    second = scan_group(values[:, 1], decay_logarithm[:, 1], keys_two, queries_two)
    mixer = jnp.stack([first, second], axis=1)
    gated = mixer * jax.nn.silu(head_gate_inputs.astype(jnp.float32)).reshape(length, 2, GROUP_HEADS, HEAD)
    scaled = gated * lax.rsqrt(lax.optimization_barrier(jnp.mean(gated * gated, axis=3, keepdims=True)) + EPSILON)
    mixed = (scaled.reshape(length, 2, CHANNELS) * head_norm_gain.astype(jnp.float32)[None]).astype(jnp.bfloat16)
    projected = jnp.dot(mixed.reshape(length, 2 * CHANNELS), output_weight.reshape(2 * CHANNELS, D), preferred_element_type=jnp.float32)
    stream = (residual.astype(jnp.float32) + projected).astype(jnp.bfloat16)
    stream_wide = stream.astype(jnp.float32)
    normed = (stream_wide * lax.rsqrt(lax.optimization_barrier(jnp.mean(stream_wide * stream_wide, axis=1, keepdims=True)) + EPSILON) * channel_norm_gain.astype(jnp.float32)[None]).astype(jnp.bfloat16)
    gate = jnp.dot(normed, channel_gate_weight, preferred_element_type=jnp.float32)
    upward = jnp.dot(normed, channel_up_weight, preferred_element_type=jnp.float32)
    hidden = (jax.nn.silu(gate) * upward).astype(jnp.bfloat16)
    block_width = FF // N_TP
    summed = jnp.zeros((length, D), jnp.float32)
    for index in range(N_TP):
        piece = hidden[:, index * block_width:(index + 1) * block_width]
        columns = channel_down_weight[:, index * block_width:(index + 1) * block_width]
        partial_value = lax.dot_general(piece, columns, (((1,), (1,)), ((), ())), preferred_element_type=jnp.float32)
        rounded = lax.optimization_barrier(partial_value.astype(jnp.bfloat16))
        summed = summed + rounded.astype(jnp.float32)
    return (stream_wide + 0.5 * summed).astype(jnp.bfloat16)
```

```python
import functools

import jax
import jax.numpy as jnp
from jax import lax
from jax.experimental import pallas as pl
from jax.experimental.pallas import tpu as pltpu
from jax.sharding import PartitionSpec as P

HEAD = 64
CONV = 4
BLOCK = 128
RIM = 16
EPSILON = 1e-06
MESH = pl.DeviceIdType.MESH


def rows_of(b):
    return pl.ds(pl.multiple_of(b * BLOCK, BLOCK), BLOCK)


def spread(columns, first, count):
    parts = [
        jnp.broadcast_to(columns[:, h : h + 1], (columns.shape[0], HEAD))
        for h in range(first, first + count)
    ]
    return jnp.concatenate(parts, axis=1)


def sigmoid(x):
    return 1.0 / (1.0 + jnp.exp(-x))


def front_kernel(
    n, tp, heads, s1, s2,
    x_ref, gate_ref, log_ref, step_ref, taps_ref, hgain_ref, wout_ref, res_ref, cgain_ref,
    normed_ref, own_ref,
    xs, rim, vals, kq, cums, st, stsend, strecv, mix, stream,
    rim_sems, st_send, st_recv, m_send, m_fwd, m_recv, r_send, r_fwd, r_recv,
):
    me = lax.axis_index("sp")
    t = lax.axis_index("tp")
    half = heads * HEAD
    wide = 2 * half
    nb = x_ref.shape[0] // BLOCK
    nx = tp // 2
    core = lax.rem(t, 2)
    my_x = t // 2
    partner = my_x * 2 + (1 - core)

    rim_copy = pltpu.make_async_remote_copy(
        src_ref=x_ref.at[pl.ds(x_ref.shape[0] - RIM, RIM)],
        dst_ref=rim,
        send_sem=rim_sems.at[0],
        recv_sem=rim_sems.at[1],
        device_id={"sp": lax.rem(me + 1, n)},
        device_id_type=MESH,
    )

    @pl.when(me < n - 1)
    def _():
        rim_copy.start()

    @pl.when(me > 0)
    def _():
        rim_copy.wait_recv()
        xs[...] = rim[...].astype(jnp.float32)[RIM - 8 :]

    @pl.when(me == 0)
    def _():
        xs[...] = jnp.zeros_like(xs)

    st[...] = jnp.zeros_like(st)
    row_i = lax.broadcasted_iota(jnp.int32, (BLOCK, BLOCK), 0)
    col_i = lax.broadcasted_iota(jnp.int32, (BLOCK, BLOCK), 1)
    causal = row_i >= col_i
    tri = jnp.where(causal, 1.0, 0.0).astype(jnp.float32)

    def state_update(b, cum):
        last = cum[BLOCK - 1 : BLOCK]
        to_end = jnp.exp(last - cum)
        decay = jnp.exp(last)
        r = rows_of(b)
        for g in range(2):
            k0, size = (wide, s1) if g == 0 else (wide + 2 * s1, s2)
            base = 0 if g == 0 else s1
            keys = kq[r, k0 - wide : k0 - wide + size]
            v = vals[r, g * half : (g + 1) * half].astype(jnp.float32)
            v = (v * spread(to_end, g * heads, heads)).astype(jnp.bfloat16)
            add = lax.dot_general(
                keys, v, (((0,), (0,)), ((), ())), preferred_element_type=jnp.float32
            )
            st[base : base + size] = (
                st[base : base + size] * spread(decay, g * heads, heads) + add
            )

    def first_pass(b, total):
        r = rows_of(b)
        current = x_ref[r].astype(jnp.float32)
        taps = taps_ref[...]
        extended = jnp.concatenate([xs[...], current], axis=0)
        acc = taps[CONV - 1 : CONV] * current
        for k in range(CONV - 1):
            acc = acc + taps[k : k + 1] * pltpu.roll(extended, CONV - 1 - k, 0)[8:]
        xs[...] = current[BLOCK - 8 :]
        acc = acc * sigmoid(acc)
        vals[r] = (acc[:, :wide] * spread(step_ref[r], 0, 2 * heads)).astype(jnp.bfloat16)
        kq[r] = acc[:, wide:].astype(jnp.bfloat16)
        cum = jnp.dot(
            tri, log_ref[r], precision=lax.Precision.HIGHEST, preferred_element_type=jnp.float32
        )
        cums[r] = cum
        state_update(b, cum)
        return total + cum[BLOCK - 1 : BLOCK]

    total = lax.fori_loop(0, nb, first_pass, jnp.zeros((1, log_ref.shape[1]), jnp.float32))

    states = s1 + s2
    stsend[0:states] = st[...].astype(jnp.bfloat16)
    which = lax.broadcasted_iota(jnp.int32, (RIM, half), 0)
    extra = jnp.zeros((RIM, half), jnp.float32)
    for g in range(2):
        logs = spread(total, g * heads, heads)
        high = logs.astype(jnp.bfloat16).astype(jnp.float32)
        low = logs - high
        extra = jnp.where(which == g, high, extra)
        extra = jnp.where(which == 2 + g, low, extra)
    stsend[states : states + RIM] = extra.astype(jnp.bfloat16)

    def state_copy(to, source):
        return pltpu.make_async_remote_copy(
            src_ref=stsend,
            dst_ref=strecv.at[source],
            send_sem=st_send.at[to],
            recv_sem=st_recv.at[source],
            device_id={"sp": to},
            device_id_type=MESH,
        )

    def send_state(to, carry):
        state_copy(to, me).start()
        return carry

    lax.fori_loop(me + 1, n, send_state, 0)
    st[...] = jnp.zeros_like(st)

    def take_state(source, carry):
        state_copy(n - 1, source).wait_recv()
        got = strecv[source].astype(jnp.float32)
        for g in range(2):
            base, size = (0, s1) if g == 0 else (s1, s2)
            logs = got[states + g : states + g + 1] + got[states + 2 + g : states + 3 + g]
            st[base : base + size] = st[base : base + size] * jnp.exp(logs) + got[base : base + size]
        return carry

    lax.fori_loop(0, me, take_state, 0)

    def share(buf, source, b, to, send, recv):
        piece = buf.at[source, rows_of(b)]
        return pltpu.make_async_remote_copy(
            src_ref=piece,
            dst_ref=piece,
            send_sem=send,
            recv_sem=recv.at[source, b],
            device_id={"tp": to},
            device_id_type=MESH,
        )

    def across(d):
        return lax.rem(my_x + d, nx) * 2

    def send_own(buf, b, send, recv):
        for d in range(1, nx):
            to = across(d) + core
            share(buf, t, b, to, send.at[d, b], recv).start()
        share(buf, t, b, partner, send.at[0, b], recv).start()

    def forward(buf, b, fwd, recv):
        for d in range(1, nx):
            source = across(d) + core
            move = share(buf, source, b, partner, fwd.at[d, b], recv)
            move.wait_recv()
            move.start()

    def wait_rest(buf, b, send, recv):
        share(buf, partner, b, partner, send.at[0, b], recv).wait_recv()
        for d in range(1, nx):
            source = across(d) + (1 - core)
            share(buf, source, b, partner, send.at[0, b], recv).wait_recv()

    def second_pass(b):
        r = rows_of(b)
        cum = cums[r]
        cum_t = cum.T
        grown = jnp.exp(cum)
        for g in range(2):
            off, size = (0, s1) if g == 0 else (2 * s1, s2)
            base = 0 if g == 0 else s1
            keys = kq[r, off : off + size]
            queries = kq[r, off + size : off + 2 * size]
            scores = lax.dot_general(
                queries, keys, (((1,), (1,)), ((), ())), preferred_element_type=jnp.float32
            )
            carried = jnp.dot(
                queries,
                st[base : base + size].astype(jnp.bfloat16),
                preferred_element_type=jnp.float32,
            )
            carried = carried * spread(grown, g * heads, heads)
            v = vals[r, g * half : (g + 1) * half]
            outs = []
            for h in range(heads):
                c = g * heads + h
                span = jnp.where(causal, cum[:, c : c + 1] - cum_t[c : c + 1, :], -jnp.inf)
                w = (jnp.exp(span) * scores).astype(jnp.bfloat16)
                lanes = slice(h * HEAD, (h + 1) * HEAD)
                y = jnp.dot(w, v[:, lanes], preferred_element_type=jnp.float32)
                y = y + carried[:, lanes]
                z = gate_ref[r, g * half + h * HEAD : g * half + (h + 1) * HEAD].astype(jnp.float32)
                y = y * (z * sigmoid(z))
                y = y * lax.rsqrt(jnp.mean(y * y, axis=1, keepdims=True) + EPSILON)
                outs.append(y)
            out = jnp.concatenate(outs, axis=1) * hgain_ref[:, g * half : (g + 1) * half]
            mix[t, r, g * half : (g + 1) * half] = out.astype(jnp.bfloat16)
        state_update(b, cum)
        send_own(mix, b, m_send, m_recv)

    def project(b):
        r = rows_of(b)
        wait_rest(mix, b, m_send, m_recv)
        acc = res_ref[r].astype(jnp.float32)
        for source in range(tp):
            acc = acc + jnp.dot(
                mix[source, r], wout_ref[source], preferred_element_type=jnp.float32
            )
        value = acc.astype(jnp.bfloat16)
        own_ref[r] = value
        stream[t, r] = value
        send_own(stream, b, r_send, r_recv)

    def normalise(b):
        r = rows_of(b)
        wait_rest(stream, b, r_send, r_recv)
        cols = own_ref.shape[1]
        parts = [stream[source, r].astype(jnp.float32) for source in range(tp)]
        square = sum(jnp.sum(p * p, axis=1, keepdims=True) for p in parts)
        scale = lax.rsqrt(square / (tp * cols) + EPSILON)
        for source in range(tp):
            lanes = slice(source * cols, (source + 1) * cols)
            normed_ref[r, lanes] = (parts[source] * scale * cgain_ref[:, lanes]).astype(
                jnp.bfloat16
            )

    def stage(b, carry):
        @pl.when(b < nb)
        def _():
            second_pass(b)

        @pl.when((b >= 1) & (b < nb + 1))
        def _():
            forward(mix, b - 1, m_fwd, m_recv)

        @pl.when((b >= 2) & (b < nb + 2))
        def _():
            project(b - 2)

        @pl.when((b >= 3) & (b < nb + 3))
        def _():
            forward(stream, b - 3, r_fwd, r_recv)

        @pl.when(b >= 4)
        def _():
            normalise(b - 4)

        return carry

    lax.fori_loop(0, nb + 4, stage, 0)

    @pl.when(me < n - 1)
    def _():
        rim_copy.wait_send()

    def end_state(to, carry):
        state_copy(to, me).wait_send()
        return carry

    lax.fori_loop(me + 1, n, end_state, 0)

    def end_shares(b, carry):
        for buf, send, fwd, recv in (
            (mix, m_send, m_fwd, m_recv),
            (stream, r_send, r_fwd, r_recv),
        ):
            for d in range(nx):
                share(buf, t, b, partner, send.at[d, b], recv).wait_send()
            for d in range(1, nx):
                share(buf, t, b, partner, fwd.at[d, b], recv).wait_send()
        return carry

    lax.fori_loop(0, nb, end_shares, 0)


def front(x, gate, logs, step, taps, hgain, wout, residual, cgain, heads, s1, s2):
    n, tp = lax.axis_size("sp"), lax.axis_size("tp")
    tokens, lanes = x.shape
    half = heads * HEAD
    cols = residual.shape[1]
    nb = tokens // BLOCK
    vmem = pl.BlockSpec(memory_space=pltpu.VMEM)
    dma = pltpu.SemaphoreType.DMA
    return pl.pallas_call(
        functools.partial(front_kernel, n, tp, heads, s1, s2),
        out_shape=(
            jax.ShapeDtypeStruct((tokens, tp * cols), jnp.bfloat16),
            jax.ShapeDtypeStruct((tokens, cols), jnp.bfloat16),
        ),
        in_specs=[vmem] * 9,
        out_specs=(vmem, vmem),
        scratch_shapes=[
            pltpu.VMEM((8, lanes), jnp.float32),
            pltpu.VMEM((RIM, lanes), jnp.bfloat16),
            pltpu.VMEM((tokens, 2 * half), jnp.bfloat16),
            pltpu.VMEM((tokens, 2 * (s1 + s2)), jnp.bfloat16),
            pltpu.VMEM((tokens, logs.shape[1]), jnp.float32),
            pltpu.VMEM((s1 + s2, half), jnp.float32),
            pltpu.VMEM((s1 + s2 + RIM, half), jnp.bfloat16),
            pltpu.VMEM((n, s1 + s2 + RIM, half), jnp.bfloat16),
            pltpu.VMEM((tp, tokens, 2 * half), jnp.bfloat16),
            pltpu.VMEM((tp, tokens, cols), jnp.bfloat16),
            dma((2,)),
            dma((n,)),
            dma((n,)),
            dma((tp, nb)),
            dma((tp, nb)),
            dma((tp, nb)),
            dma((tp, nb)),
            dma((tp, nb)),
            dma((tp, nb)),
        ],
        compiler_params=pltpu.CompilerParams(has_side_effects=True, vmem_limit_bytes=56 << 20),
        name="front",
    )(x, gate, logs, step, taps, hgain, wout, residual, cgain)


def shards(
    grouped_head_inputs,
    head_gate_inputs,
    unsmoothed_step,
    head_decay_rate,
    extra_log_decay,
    first_group_keys,
    first_group_queries,
    second_group_keys,
    second_group_queries,
    head_input_filter,
    first_group_filter,
    second_group_filter,
    head_norm_gain,
    output_weight,
    residual,
    channel_norm_gain,
    channel_gate_weight,
    channel_up_weight,
    channel_down_weight,
):
    tp = lax.axis_size("tp")
    tokens = grouped_head_inputs.shape[0]
    heads = head_decay_rate.shape[1]
    half = heads * HEAD
    s1, s2 = first_group_keys.shape[1], second_group_keys.shape[1]
    gate_full = lax.all_gather(channel_gate_weight, "sp", axis=0, tiled=True)
    up_full = lax.all_gather(channel_up_weight, "sp", axis=0, tiled=True)
    down_full = lax.all_gather(channel_down_weight, "sp", axis=0, tiled=True)
    x = jnp.concatenate(
        [
            grouped_head_inputs.reshape(tokens, 2 * half),
            first_group_keys,
            first_group_queries,
            second_group_keys,
            second_group_queries,
        ],
        axis=1,
    )
    taps = jnp.concatenate(
        [
            head_input_filter.reshape(CONV, 2 * half),
            first_group_filter.reshape(CONV, 2 * s1),
            second_group_filter.reshape(CONV, 2 * s2),
        ],
        axis=1,
    )
    step = jax.nn.softplus(unsmoothed_step.reshape(tokens, 2 * heads))
    logs = extra_log_decay.reshape(tokens, 2 * heads) - step * head_decay_rate.reshape(1, -1)
    pad = ((0, 0), (0, BLOCK - 2 * heads))
    wout = output_weight.reshape(2, tp, half, -1).swapaxes(0, 1).reshape(tp, 2 * half, -1)
    normed, stream = front(
        x,
        head_gate_inputs.reshape(tokens, 2 * half),
        jnp.pad(logs, pad),
        jnp.pad(step, pad),
        taps,
        head_norm_gain.reshape(1, 2 * half),
        wout,
        residual,
        channel_norm_gain.reshape(1, -1),
        heads,
        s1,
        s2,
    )
    gate = jnp.dot(normed, gate_full, preferred_element_type=jnp.float32)
    upward = jnp.dot(normed, up_full, preferred_element_type=jnp.float32)
    hidden = (jax.nn.silu(gate) * upward).astype(jnp.bfloat16)
    partial_value = lax.dot_general(
        hidden, down_full, (((1,), (1,)), ((), ())), preferred_element_type=jnp.float32
    )
    summed = lax.psum_scatter(
        partial_value.astype(jnp.bfloat16), "tp", scatter_dimension=1, tiled=True
    ).astype(jnp.float32)
    return (stream.astype(jnp.float32) + 0.5 * summed).astype(jnp.bfloat16)


def solution(mesh):
    return jax.shard_map(
        shards,
        mesh=mesh,
        in_specs=(
            P("sp", None, "tp"),
            P("sp", None, "tp"),
            P("sp", None, "tp"),
            P(None, "tp"),
            P("sp", None, "tp"),
            P("sp", None),
            P("sp", None),
            P("sp", None),
            P("sp", None),
            P(None, None, "tp"),
            P(),
            P(),
            P(None, "tp"),
            P(None, None, "tp"),
            P("sp", "tp"),
            P(),
            P("sp", "tp"),
            P("sp", "tp"),
            P("sp", "tp"),
        ),
        out_specs=P("sp", "tp"),
        check_vma=False,
    )
```
